128 devices in a mesh: sp: 64 (over z, y, x), tp: 2 (over core).
Axes of the slice: x: 4, y: 4, z: 4, core: 2. Of those that a mesh axis runs over, the one named last changes fastest.
Arguments:
- residual: bfloat16 [8192, 2048], P(('sp', 'tp')), may hold values from -6 to 6
- conv_input: bfloat16 [8192, 1024], P('sp', 'tp'), may hold values from -6 to 6
- input_gate: bfloat16 [8192, 1024], P('sp', 'tp'), may hold values from -6 to 6
- output_gate: bfloat16 [8192, 1024], P('sp', 'tp'), may hold values from -6 to 6
- conv_taps: bfloat16 [3, 1024], P(None, 'tp'), may hold values from -3.5 to 3.5
- out_proj: bfloat16 [1024, 2048], P('tp'), may hold values from -0.1875 to 0.1875
- norm_gain: float32 [2048], replicated, may hold values from 0.1 to 1.9
- routes: int32 [8192, 2], P(('sp', 'tp')), may hold values from 0 to 63, all different within a row; in each aligned block of 64 rows (0 to 63, 64 to 127, ...) at most 4 rows name the same one
- route_weight: float32 [8192, 2], P(('sp', 'tp')), may hold values from 0.1 to 1
- gate_proj: bfloat16 [64, 2048, 3584], P('sp', None, 'tp'), may hold values from -0.125 to 0.125
- up_proj: bfloat16 [64, 2048, 3584], P('sp', None, 'tp'), may hold values from -0.125 to 0.125
- down_proj: bfloat16 [64, 3584, 2048], P('sp', 'tp'), may hold values from -0.09375 to 0.09375
Outputs:
- layer_out: bfloat16 [8192, 2048], P(('sp', 'tp'))
The draws below stay inside these ranges and needn't reach their ends.
Inputs may be any that keep to these rules, and one draw needn't show every extreme that they name: `routes`: A token's 2 experts differ. Among the 64 tokens of one device, in the aligned blocks of the tokens' order, no expert is named more than 4 times, a bound that some block reaches in some device.
All inputs are finite; a program needn't handle non-finite values.
Results may differ from the reference program's by a relative error of at most 0.0054.
Values may be sent and summed in bfloat16 or wider, within the bound.
A program may use at most 128 MiB of HBM per device.

```python
import math
import jax
import jax.numpy as jnp
import numpy as np
from jax import lax

D = 2048
CW = 1024
FF = 3584
KSIZE = 3
TOPK = 2
TOK_SH = 64
TOKENS = 8192
EXPERTS = 64
CAP = 4
N_SP = 64
N_TP = 2


def level_of(key, dims, cuts, smallest, largest):
    gain, own = 1.0, jax.random.fold_in(key, 6)
    for position, blocks in cuts:
        steps = jnp.exp(jax.random.uniform(jax.random.fold_in(own, position), (blocks,), jnp.float32, smallest / len(cuts), largest / len(cuts)))
        gain = gain * jnp.repeat(steps, dims[position] // blocks).reshape([-1 if axis == position else 1 for axis in range(len(dims))])
    return gain


def routed_block(key, own, number, rows, count, top, limit, lean):
    order = jax.random.permutation(key, count)
    packed, usual = load_shares(count, rows * top, limit, lean, True), load_shares(count, rows * top, limit, lean, False)
    places = jnp.arange(count)

    def named(lengths, rotation):
        used = int((lengths > 0).sum())
        fixed = max(1, used // 4)
        passed = fixed + (places - fixed + rotation * (used - fixed)) % max(1, count - fixed)
        return jnp.zeros((count,), jnp.int32).at[order[jnp.where(places < fixed, places, passed)]].set(jnp.asarray(lengths, jnp.int32))

    lengths = jnp.where(number % 4 == 0, named(packed, number // 4), named(usual, number - number // 4 - 1))
    mixed = jax.random.permutation(jax.random.fold_in(own, 3), count)
    donor, receiver = mixed[0:count // 2 * 2:2], mixed[1:count // 2 * 2:2]
    margin = jnp.minimum(lengths[donor] - 1, limit - lengths[receiver]) // 2
    margin = jnp.where((donor == order[0]) | (receiver == order[0]) | (lengths[receiver] == 0), 0, jnp.maximum(margin, 0))
    passed = jax.random.randint(jax.random.fold_in(own, 4), (count // 2,), 0, 1 << 20) % (margin + 1)
    lengths = lengths.at[donor].add(-passed).at[receiver].add(passed)
    items = jnp.searchsorted(jnp.cumsum(lengths), jnp.arange(rows * top), side="right").astype(jnp.int32)
    table = items.reshape(top, rows).T
    table = table[jax.random.permutation(jax.random.fold_in(own, 1), rows)]
    rotation = jax.random.randint(jax.random.fold_in(own, 2), (rows, 1), 0, top)
    return jnp.take_along_axis(table, (jnp.arange(top)[None, :] + rotation) % top, axis=1)


def load_shares(amount, total, limit, lean, full):
    portions = [(1 << 20) // math.isqrt(rank ** lean) + 1 for rank in range(1, amount + 1)]
    largest = limit if full else min(limit, max(-(-total // amount), total * portions[0] // sum(portions)))
    least = 1 if total - largest >= amount - 1 else 0
    given, spare = [largest] + [least] * (amount - 1), total - largest - least * (amount - 1)
    while spare > 0:
        movable = [i for i in range(1, amount) if given[i] < largest] or [i for i in range(1, amount) if given[i] < limit]
        pool, budget = sum([portions[i] for i in movable]), spare
        for i in movable:
            addition = min(limit - given[i], max(1, budget * portions[i] // pool), spare)
            given[i] = given[i] + addition
            spare = spare - addition
    return np.array(given)


def centred(stream_key, extent, scale, limit, pieces=(), kind=jnp.bfloat16):
    entries = scale * jax.random.normal(stream_key, extent, jnp.float32)
    if pieces:
        entries = entries * level_of(stream_key, extent, pieces, -0.22, 0.18)
    return jnp.clip(entries, -limit, limit).astype(kind)


def setup_inputs(seed: int = 0) -> dict:
    streams_of = jax.random.split(jax.random.key(seed), 13)
    residual = centred(streams_of[0], (TOKENS, D), 1.0, 6.0, ((0, 128),))
    conv_input = centred(streams_of[1], (TOKENS, CW), 1.0, 6.0, ((0, 64), (1, 2)))
    input_gate = centred(streams_of[2], (TOKENS, CW), 1.0, 6.0, ((0, 64), (1, 2)))
    output_gate = centred(streams_of[3], (TOKENS, CW), 1.0, 6.0, ((0, 64), (1, 2)))
    conv_taps = centred(streams_of[4], (KSIZE, CW), KSIZE ** -0.5, 3.5, ((1, 2),))
    out_proj = centred(streams_of[5], (CW, D), CW ** -0.5, 0.1875, ((0, 2),))
    norm_gain = jnp.clip(1.0 + 0.18 * jax.random.normal(streams_of[6], (D,), jnp.float32), 0.1, 1.9)
    routes_keys = jax.random.split(jax.random.fold_in(streams_of[7], 1), TOKENS // TOK_SH)
    routes_turns = jax.random.permutation(jax.random.fold_in(streams_of[7], 3), TOKENS // TOK_SH)
    routes = jax.vmap(lambda own, number: routed_block(jax.random.fold_in(streams_of[7], 2), own, number, TOK_SH, EXPERTS, TOPK, CAP, 2))(routes_keys, routes_turns).reshape((TOKENS, TOPK))
    route_weight = jnp.clip(0.1 + 0.9 * jax.random.uniform(streams_of[8], (TOKENS, TOPK), jnp.float32) ** level_of(streams_of[8], (TOKENS, TOPK), ((0, 128),), -0.2, 0.2), 0.1, 1.0)
    gate_proj = centred(streams_of[9], (EXPERTS, D, FF), D ** -0.5, 0.125, ((0, 64), (2, 2)))
    up_proj = centred(streams_of[10], (EXPERTS, D, FF), D ** -0.5, 0.125, ((0, 64), (2, 2)))
    down_proj = centred(streams_of[11], (EXPERTS, FF, D), FF ** -0.5, 0.09375, ((0, 64), (1, 2)))
    return {"residual": residual, "conv_input": conv_input, "input_gate": input_gate, "output_gate": output_gate, "conv_taps": conv_taps, "out_proj": out_proj, "norm_gain": norm_gain, "routes": routes, "route_weight": route_weight, "gate_proj": gate_proj, "up_proj": up_proj, "down_proj": down_proj}


def reference(residual, conv_input, input_gate, output_gate, conv_taps, out_proj, norm_gain, routes, route_weight, gate_proj, up_proj, down_proj):
    tap_count = conv_taps.shape[0]
    length = conv_input.shape[0]
    mixed = input_gate.astype(jnp.float32) * conv_input.astype(jnp.float32)
    padded = jnp.pad(mixed, ((tap_count - 1, 0), (0, 0)))
    convolved = jnp.zeros_like(mixed)
    for tap_index in range(tap_count):
        convolved = convolved + conv_taps[tap_index].astype(jnp.float32)[None, :] * padded[tap_index:tap_index + length]
    gated_rows = (output_gate.astype(jnp.float32) * convolved).astype(jnp.bfloat16)
    stream = residual.astype(jnp.float32) + jnp.dot(gated_rows, out_proj, preferred_element_type=jnp.float32)
    inverse_rms = lax.rsqrt(lax.optimization_barrier(jnp.mean(stream * stream, axis=-1, keepdims=True)) + 1e-06)
    normed = (stream * inverse_rms * norm_gain.astype(jnp.float32)[None, :]).astype(jnp.bfloat16)
    blocks = N_SP * N_TP
    tok_rows = TOKENS // blocks
    per_block = tok_rows * TOPK
    flat_routes = routes.reshape(blocks, per_block)
    onehot = (flat_routes[:, :, None] == jnp.arange(EXPERTS, dtype=jnp.int32)[None, None, :]).astype(jnp.int32)
    counts = jnp.cumsum(onehot, axis=1)
    slot_ids = lax.optimization_barrier(jnp.sum(onehot * (counts - 1), axis=2)).astype(jnp.int32)
    token_ids = (jnp.arange(blocks * per_block, dtype=jnp.int32) // TOPK).reshape(blocks, per_block)
    block_ids = jnp.broadcast_to(jnp.arange(blocks, dtype=jnp.int32)[:, None], (blocks, per_block))
    slot_table = jnp.zeros((EXPERTS, blocks, CAP), jnp.int32).at[flat_routes, block_ids, slot_ids].set(token_ids)
    weight_table = jnp.zeros((EXPERTS, blocks, CAP), jnp.float32).at[flat_routes, block_ids, slot_ids].set(route_weight.astype(jnp.float32).reshape(blocks, per_block))
    half_width = FF // N_TP

    def expert_step(running, inputs):
        ids_here, weights_here, gate_part, up_part, down_part = inputs
        flat_ids = ids_here.reshape(-1)
        flat_rows = normed[flat_ids]
        summed = jnp.zeros((flat_rows.shape[0], flat_rows.shape[1]), jnp.float32)
        for half_index in range(N_TP):
            lower = half_index * half_width
            upper = lower + half_width
            gate_val = jnp.dot(flat_rows, gate_part[:, lower:upper], preferred_element_type=jnp.float32)
            up_val = jnp.dot(flat_rows, up_part[:, lower:upper], preferred_element_type=jnp.float32)
            active = (jax.nn.silu(gate_val) * up_val).astype(jnp.bfloat16)
            partial_value = jnp.dot(active, down_part[lower:upper], preferred_element_type=jnp.float32).astype(jnp.bfloat16)
            partial_value = lax.optimization_barrier(partial_value)
            summed = summed + partial_value.astype(jnp.float32)
        halves = lax.optimization_barrier(summed.astype(jnp.bfloat16))
        running = running.at[flat_ids].add(weights_here.reshape(-1)[:, None] * halves.astype(jnp.float32))
        return (running, None)
    routed, _ = lax.scan(expert_step, jnp.zeros((TOKENS, D), jnp.float32), (slot_table, weight_table, gate_proj, up_proj, down_proj))
    return (stream + routed).astype(jnp.bfloat16)
```

```python
import functools

import jax
import jax.numpy as jnp
from jax import lax
from jax.experimental import pallas as pl
from jax.experimental.pallas import tpu as pltpu
from jax.sharding import PartitionSpec as P

MESH = pl.DeviceIdType.MESH
F32, BF16, I32 = jnp.float32, jnp.bfloat16, jnp.int32
SIDE = 4
GROUPS = 4
SLABS = 16
SLOTS = 4
QUARTERS = 4
ROWS = SLABS * QUARTERS * SLOTS
EPS = 1e-06


def ring_distance(a):
    return min(a, SIDE - a)


def offsets_far_first(g):
    found = [(dz, dy, (g - dz - dy) % SIDE) for dz in range(SIDE) for dy in range(SIDE)]
    return sorted(found, key=lambda o: -sum(ring_distance(a) for a in o))


def iota(shape, dim):
    return lax.broadcasted_iota(I32, shape, dim)


def dot(a, b):
    return jnp.dot(a, b, preferred_element_type=F32)


def kernel(
    res_h, cin_h, gin_h, gout_h, taps_ref, oproj_h, gain_ref, routes_ref, weight_ref,
    wg_h, wu_h, wd_h, out_ref,
    cin_v, gin_v, gout_v, res_v, op_v, wg_v, wu_v, wd_v, halo, part, pxr, stream, n4,
    send, rown, roth, rsend, rret, x_v, h_v, yown, pps, ppr, u_v, ut_v, comb,
    in_sem, w_sem, halo_s, halo_r, px_s, px_r, dsp_s, dsp_r, fwd_s, fwd_r, pp_s, pp_r, ret_s, ret_r,
):
    sp, tp = lax.axis_index("sp"), lax.axis_index("tp")
    z, y, x = lax.div(sp, 16), lax.rem(lax.div(sp, 4), 4), lax.rem(sp, 4)
    other = 1 - tp
    rows, tok = cin_v.shape[0], res_v.shape[0]
    width, hidden = out_ref.shape[1], h_v.shape[1]
    piece = width // QUARTERS

    def remote(src, dst, s, r, **where):
        return pltpu.make_async_remote_copy(
            src_ref=src, dst_ref=dst, send_sem=s, recv_sem=r, device_id=where, device_id_type=MESH
        )

    loads = [
        pltpu.make_async_copy(a, b, in_sem.at[i])
        for i, (a, b) in enumerate(
            [(cin_h, cin_v), (gin_h, gin_v), (gout_h, gout_v), (oproj_h, op_v), (res_h, res_v)]
        )
    ]
    for load in loads:
        load.start()

    barrier = pltpu.get_barrier_semaphore()
    peers = SIDE**3

    def greet(i, carry):
        pl.semaphore_signal(
            barrier, inc=1, device_id={"sp": lax.rem(sp + i + 1, peers)}, device_id_type=MESH
        )
        return carry

    lax.fori_loop(0, peers - 1, greet, 0)
    pl.semaphore_signal(barrier, inc=1, device_id={"tp": other}, device_id_type=MESH)

    def weight_copies(i, src, dst, cuts):
        size = dst.shape[0] // cuts
        return [
            pltpu.make_async_copy(
                src.at[0, pl.ds(k * size, size)], dst.at[pl.ds(k * size, size)], w_sem.at[i]
            )
            for k in range(cuts)
        ]

    for i, (src, dst) in enumerate([(wg_h, wg_v), (wu_h, wu_v), (wd_h, wd_v)]):
        for copy in weight_copies(i, src, dst, 4):
            copy.start()

    routes = routes_ref[...].astype(F32)
    r0c, r1c = routes[:, 0:1], routes[:, 1:2]
    lanes = QUARTERS * tok
    trow, tcol = iota((tok, lanes), 0), lax.rem(iota((tok, lanes), 1), tok)
    same, before = trow == tcol, trow < tcol
    keys = []
    for rc in (r0c, r1c):
        rrow = jnp.sum(jnp.where(same, rc, 0.0), axis=0, keepdims=True)
        hits = ((r0c == rrow) | (r1c == rrow)) & before
        rank = jnp.sum(jnp.where(hits, 1.0, 0.0), axis=0, keepdims=True).astype(I32)
        e = rrow.astype(I32)
        dz = (lax.shift_right_logical(e, 4) + SIDE - z) & 3
        dy = ((lax.shift_right_logical(e, 2) & 3) + SIDE - y) & 3
        dx = ((e & 3) + SIDE - x) & 3
        keys.append((((dz + dy + dx) & 3) * SLABS + dz * SIDE + dy) * SLOTS + rank)
    first = trow == iota((tok, lanes), 1)
    key_cols = [
        jnp.sum(jnp.where(first, k.astype(F32), 0.0), axis=1, keepdims=True).astype(I32) for k in keys
    ]

    a, b = iota((ROWS, ROWS), 0), iota((ROWS, ROWS), 1)

    def plain_to_slab(r):
        q, i, s = lax.shift_right_logical(r, 6), lax.shift_right_logical(r, 2) & 15, r & 3
        return i * 16 + q * 4 + s

    u_v[...] = jnp.where(plain_to_slab(a) == b, 1.0, 0.0).astype(BF16)
    ut_v[...] = jnp.where(plain_to_slab(b) == a, 1.0, 0.0).astype(BF16)

    taps = taps_ref[...].astype(F32)
    t0, t1, t2 = taps[0:1], taps[1:2], taps[2:3]
    for load in loads[:3]:
        load.wait()
    mixed = gin_v[...].astype(F32) * cin_v[...].astype(F32)
    row = iota(mixed.shape, 0)
    m1 = jnp.where(row < 1, 0.0, pltpu.roll(mixed, 1, 0))
    m2 = jnp.where(row < 2, 0.0, pltpu.roll(mixed, 2, 0))
    gated = (gout_v[...].astype(F32) * (t0 * m2 + t1 * m1 + t2 * mixed)).astype(BF16)
    loads[3].wait()
    part[...] = dot(gated, op_v[...])

    pl.semaphore_wait(barrier, peers)
    behind = lax.rem(sp + 1, peers)
    halos = [
        remote(v.at[pl.ds(rows - 16, 16)], halo.at[i], halo_s.at[i], halo_r.at[i], sp=behind)
        for i, v in enumerate((cin_v, gin_v))
    ]
    for copy in halos:
        copy.start()
    theirs = pl.multiple_of(other * tok, tok)
    spans = [(0, 16), (16, tok - 16)]
    swaps = [
        remote(
            part.at[pl.ds(pl.multiple_of(theirs + lo, 16), n)], pxr.at[pl.ds(lo, n)],
            px_s.at[i], px_r.at[i], tp=other,
        )
        for i, (lo, n) in enumerate(spans)
    ]
    swaps[1].start()
    for copy in halos:
        copy.wait()
    hm = jnp.where(sp > 0, halo[0].astype(F32) * halo[1].astype(F32), 0.0)
    ext = jnp.concatenate([hm, gin_v[0:16].astype(F32) * cin_v[0:16].astype(F32)], axis=0)
    conv = t0 * pltpu.roll(ext, 2, 0)[16:32] + t1 * pltpu.roll(ext, 1, 0)[16:32] + t2 * ext[16:32]
    part[0:16] = dot((gout_v[0:16].astype(F32) * conv).astype(BF16), op_v[...])
    swaps[0].start()
    loads[4].wait()
    for copy in swaps:
        copy.wait()
    s = part[pl.ds(pl.multiple_of(tp * tok, tok), tok)] + pxr[...] + res_v[...].astype(F32)
    stream[...] = s
    inverse = lax.rsqrt(jnp.mean(s * s, axis=-1, keepdims=True) + EPS)
    normed = (s * inverse * gain_ref[...]).astype(BF16)
    for q in range(QUARTERS):
        n4[q * tok : (q + 1) * tok] = normed[:, q * piece : (q + 1) * piece]

    def peer(sign, dz, dy, dx):
        return (
            lax.rem(z + (sign * dz) % SIDE, SIDE) * 16
            + lax.rem(y + (sign * dy) % SIDE, SIDE) * 4
            + lax.rem(x + (sign * dx) % SIDE, SIDE)
        )

    slab_of = lax.shift_right_logical(a, 4) * SLOTS + (a & 3)
    quarter_ok = (lax.shift_right_logical(a, 2) & 3) == lax.shift_right_logical(b, 6)
    for g in range(GROUPS):
        want = slab_of + g * SLABS * SLOTS
        pick = jnp.where(((keys[0] == want) | (keys[1] == want)) & quarter_ok, 1.0, 0.0).astype(BF16)
        send[g * SLABS : (g + 1) * SLABS] = dot(pick, n4[...]).astype(BF16).reshape(SLABS, 16, piece)
        for dz, dy, dx in offsets_far_first(g):
            pos = g * SLABS + dz * SIDE + dy
            if pos:
                remote(send.at[pos], rown.at[pos], dsp_s, dsp_r.at[g], sp=peer(1, dz, dy, dx)).start()
            else:
                pltpu.make_async_copy(send.at[0], rown.at[0], dsp_r.at[0]).start()

    def group(ref, g):
        return ref.at[pl.ds(g * SLABS, SLABS)]

    def forward(g):
        return remote(group(rown, g), group(roth, g), fwd_s.at[g], fwd_r.at[g], tp=other)

    def arrived(ref, sems, g):
        return remote(group(ref, g), group(ref, g), sems.at[g], sems.at[g], tp=other)

    def halves(g):
        return remote(pps.at[g], ppr.at[g], pp_s.at[g], pp_r.at[g], tp=other)

    arrived(rown, dsp_r, 0).wait_recv()
    forward(0).start()
    for i, (src, dst) in enumerate([(wg_h, wg_v), (wu_h, wu_v), (wd_h, wd_v)]):
        pltpu.make_async_copy(src.at[0], dst, w_sem.at[i]).wait()

    by_plane = sorted(
        [(dz, dy) for dz in range(SIDE) for dy in range(SIDE)],
        key=lambda o: -sum(ring_distance(k) for k in o),
    )

    def expert(g, carry):
        forward(g).wait_recv()
        for half, ref in enumerate((rown, roth)):
            slabs = ref[pl.ds(g * SLABS, SLABS)].reshape(ROWS, piece)
            plain = dot(u_v[...], slabs).astype(BF16)
            for q in range(QUARTERS):
                x_v[half * tok : (half + 1) * tok, q * piece : (q + 1) * piece] = plain[
                    q * tok : (q + 1) * tok
                ]
        for n in range(hidden // 256):
            cols = slice(n * 256, (n + 1) * 256)
            gate, up = dot(x_v[...], wg_v[:, cols]), dot(x_v[...], wu_v[:, cols])
            h_v[:, cols] = (gate / (1.0 + jnp.exp(-gate)) * up).astype(BF16)
        for q in range(QUARTERS):
            cols = slice(q * piece, (q + 1) * piece)
            res = dot(h_v[...], wd_v[:, cols]).astype(BF16)
            yown[q * tok : (q + 1) * tok] = res[:tok]
            pps[g, q * tok : (q + 1) * tok] = res[tok:]
        halves(g).start()

        @pl.when(g < GROUPS - 1)
        def _():
            arrived(rown, dsp_r, g + 1).wait_recv()
            forward(g + 1).start()

        halves(g).wait_recv()
        total = (yown[...].astype(F32) + ppr[g].astype(F32)).astype(BF16)
        rsend[pl.ds(g * SLABS, SLABS)] = dot(ut_v[...], total).astype(BF16).reshape(SLABS, 16, piece)
        for dz, dy in by_plane:
            pos = g * SLABS + dz * SIDE + dy
            dx = lax.rem(g + 2 * SIDE - dz - dy, SIDE)
            dst = (
                lax.rem(z + SIDE - dz, SIDE) * 16
                + lax.rem(y + SIDE - dy, SIDE) * 4
                + lax.rem(x + SIDE - dx, SIDE)
            )

            def back(pos=pos, dst=dst):
                remote(rsend.at[pos], rret.at[pos], ret_s, ret_r.at[g], sp=dst).start()

            if dz or dy:
                back()
            else:
                pl.when(g > 0)(back)

                @pl.when(g == 0)
                def _():
                    pltpu.make_async_copy(rsend.at[0], rret.at[0], ret_r.at[0]).start()

        return carry

    lax.fori_loop(0, GROUPS, expert, 0)

    lane = iota((tok, ROWS), 1)
    lane_slot = lax.shift_right_logical(lane, 4) * SLOTS + (lane & 3)
    lane_quarter = lax.shift_right_logical(lane, 2) & 3
    weights = weight_ref[...]
    w0, w1 = weights[:, 0:1], weights[:, 1:2]
    comb[...] = jnp.zeros_like(comb)

    def combine(g, carry):
        want = lane_slot + g * SLABS * SLOTS
        mix = jnp.where(key_cols[0] == want, w0, 0.0) + jnp.where(key_cols[1] == want, w1, 0.0)
        high = mix.astype(BF16).astype(F32)
        low = mix - high
        pieces = [
            jnp.where(lane_quarter == q, m, 0.0).astype(BF16) for m in (high, low) for q in range(QUARTERS)
        ]
        arrived(rret, ret_r, g).wait_recv()
        slabs = rret[pl.ds(g * SLABS, SLABS)].reshape(ROWS, piece)
        comb[...] += dot(jnp.concatenate(pieces, axis=0), slabs)
        return carry

    lax.fori_loop(0, GROUPS, combine, 0)
    for q in range(QUARTERS):
        cols = slice(q * piece, (q + 1) * piece)
        routed = comb[q * tok : (q + 1) * tok] + comb[(QUARTERS + q) * tok : (QUARTERS + q + 1) * tok]
        out_ref[:, cols] = (stream[:, cols] + routed).astype(BF16)

    rest = pl.ds(1, GROUPS * SLABS - 1)
    remote(send.at[rest], rown.at[rest], dsp_s, dsp_s, tp=other).wait_send()
    remote(rsend.at[rest], rret.at[rest], ret_s, ret_s, tp=other).wait_send()
    for g in range(GROUPS):
        forward(g).wait_send()
        halves(g).wait_send()


def per_device(
    residual, conv_input, input_gate, output_gate, conv_taps, out_proj, norm_gain, routes,
    route_weight, gate_proj, up_proj, down_proj,
):
    rows, chan = conv_input.shape
    tok, width = residual.shape
    hidden = gate_proj.shape[2]
    piece = width // QUARTERS
    slabs = (GROUPS * SLABS, QUARTERS * SLOTS, piece)
    anyspace = pl.BlockSpec(memory_space=pl.ANY)
    vmem = pl.BlockSpec(memory_space=pltpu.VMEM)
    dma = pltpu.SemaphoreType.DMA
    v = pltpu.VMEM
    return pl.pallas_call(
        kernel,
        out_shape=jax.ShapeDtypeStruct((tok, width), BF16),
        in_specs=[
            anyspace, anyspace, anyspace, anyspace, vmem, anyspace, vmem, vmem, vmem,
            anyspace, anyspace, anyspace,
        ],
        out_specs=vmem,
        scratch_shapes=[
            v((rows, chan), BF16), v((rows, chan), BF16), v((rows, chan), BF16),
            v((tok, width), BF16), v((chan, width), BF16),
            v((width, hidden), BF16), v((width, hidden), BF16), v((hidden, width), BF16),
            v((2, 16, chan), BF16), v((rows, width), F32), v((tok, width), F32), v((tok, width), F32),
            v((QUARTERS * tok, piece), BF16),
            v(slabs, BF16), v(slabs, BF16), v(slabs, BF16), v(slabs, BF16), v(slabs, BF16),
            v((2 * tok, width), BF16), v((2 * tok, hidden), BF16), v((ROWS, piece), BF16),
            v((GROUPS, ROWS, piece), BF16), v((GROUPS, ROWS, piece), BF16),
            v((ROWS, ROWS), BF16), v((ROWS, ROWS), BF16), v((2 * ROWS, piece), F32),
            dma((5,)), dma((3,)), dma((2,)), dma((2,)), dma((2,)), dma((2,)),
            dma, dma((GROUPS,)), dma((GROUPS,)), dma((GROUPS,)), dma((GROUPS,)), dma((GROUPS,)),
            dma, dma((GROUPS,)),
        ],
        compiler_params=pltpu.CompilerParams(
            collective_id=0, has_side_effects=True, vmem_limit_bytes=60 * 2**20
        ),
        name="layer",
    )(
        residual, conv_input, input_gate, output_gate, conv_taps, out_proj, norm_gain.reshape(1, -1),
        routes, route_weight, gate_proj, up_proj, down_proj,
    )


def solution(mesh):
    return jax.shard_map(
        per_device,
        mesh=mesh,
        in_specs=(
            P(("sp", "tp"), None),
            P("sp", "tp"),
            P("sp", "tp"),
            P("sp", "tp"),
            P(None, "tp"),
            P("tp", None),
            P(),
            P(("sp", "tp"), None),
            P(("sp", "tp"), None),
            P("sp", None, "tp"),
            P("sp", None, "tp"),
            P("sp", "tp", None),
        ),
        out_specs=P(("sp", "tp"), None),
        check_vma=False,
    )
```

```python
import functools

import jax
import jax.numpy as jnp
from jax import lax
from jax.experimental import pallas as pl
from jax.experimental.pallas import tpu as pltpu
from jax.sharding import PartitionSpec as P

MESH = pl.DeviceIdType.MESH
F32, BF16, I32 = jnp.float32, jnp.bfloat16, jnp.int32
SIDE = 4
GROUPS = 4
SLABS = 16
SLOTS = 4
QUARTERS = 4
ROWS = SLABS * QUARTERS * SLOTS
EPS = 1e-06


def distance(offset):
    return sum(min(k, SIDE - k) for k in offset)


def peer_groups():
    every = [(i, j, k) for i in range(SIDE) for j in range(SIDE) for k in range(SIDE)]
    one_way = [o for o in every if distance(o) == 2 and (2 in o or set(o) in ({0, 1}, {0, 3}))]
    first = [o for o in every if distance(o) < 2] + one_way
    second = [o for o in every if distance(o) == 2 and o not in one_way]
    second += [o for o in every if distance(o) == 3 and 2 not in o] + [(2, 1, 0), (2, 3, 0)]
    far = sorted((o for o in every if o not in first and o not in second), key=distance)
    return [first, second, far[0::2], far[1::2]]


PEERS = peer_groups()
PLACE = {o: g * SLABS + i for g, members in enumerate(PEERS) for i, o in enumerate(members)}


def far_first(g):
    return sorted(PEERS[g], key=lambda o: -distance(o))


def iota(shape, dim):
    return lax.broadcasted_iota(I32, shape, dim)


def dot(a, b):
    return jnp.dot(a, b, preferred_element_type=F32)


def kernel(
    res_h, cin_h, gin_h, gout_h, taps_h, oproj_h, gain_h, routes_h, weight_h,
    wg_h, wu_h, wd_h, out_ref,
    taps_ref, gain_ref, routes_ref, weight_ref, cin_v, gin_v, gout_v, res_v, op_v, wg_v, wu_v, wd_v, halo, part, pxr, stream, n4,
    send, taken, rsend, rret, x_v, h_v, mine, theirs, u_v, ut_v, picks, mixes, comb,
    known, in_sem, w_sem, halo_s, halo_r, px_s, px_r, dsp_s, dsp_r, fwd_s, fwd_r, pp_s, pp_r, ret_s, ret_r,
):
    sp, tp = lax.axis_index("sp"), lax.axis_index("tp")
    z, y, x = lax.div(sp, 16), lax.rem(lax.div(sp, 4), 4), lax.rem(sp, 4)
    other = 1 - tp
    rows, tok = cin_v.shape[0], res_v.shape[0]
    width, hidden = out_ref.shape[1], h_v.shape[1]
    piece = width // QUARTERS

    def remote(src, dst, s, r, **where):
        return pltpu.make_async_remote_copy(
            src_ref=src, dst_ref=dst, send_sem=s, recv_sem=r, device_id=where, device_id_type=MESH
        )

    def peer(offset, sign=1):
        dz, dy, dx = (sign * k % SIDE for k in offset)
        return lax.rem(z + dz, SIDE) * 16 + lax.rem(y + dy, SIDE) * 4 + lax.rem(x + dx, SIDE)

    barrier = pltpu.get_barrier_semaphore()
    peers = SIDE**3
    lines = [[tuple(k if a == axis else 0 for a in range(3)) for k in range(1, SIDE)] for axis in range(3)]
    for line in lines:
        for offset in line:
            pl.semaphore_signal(barrier, inc=1, device_id={"sp": peer(offset)}, device_id_type=MESH)
    pl.semaphore_signal(barrier, inc=1, device_id={"tp": other}, device_id_type=MESH)
    pl.semaphore_signal(
        barrier, inc=1, device_id={"sp": lax.rem(sp + peers - 1, peers)}, device_id_type=MESH
    )

    loads = [
        pltpu.make_async_copy(a, b, in_sem.at[i])
        for i, (a, b) in enumerate(
            [
                (routes_h, routes_ref), (cin_h, cin_v), (gin_h, gin_v), (gout_h, gout_v),
                (taps_h, taps_ref), (oproj_h, op_v), (res_h, res_v), (gain_h, gain_ref),
                (weight_h, weight_ref),
            ]
        )
    ]
    for load in loads:
        load.start()
    lanes = QUARTERS * tok
    trow, tcol = iota((tok, lanes), 0), lax.rem(iota((tok, lanes), 1), tok)
    same, before = trow == tcol, trow < tcol
    loads[0].wait()
    diagonal = iota((tok, tok), 0) == iota((tok, tok), 1)

    def upright(line):
        return jnp.sum(jnp.where(diagonal, line, 0.0), axis=1, keepdims=True)

    cols = [upright(routes_ref[k : k + 1].astype(F32)) for k in range(2)]
    keys = []
    for rc in cols:
        rrow = jnp.sum(jnp.where(same, rc, 0.0), axis=0, keepdims=True)
        hits = ((cols[0] == rrow) | (cols[1] == rrow)) & before
        rank = jnp.sum(jnp.where(hits, 1.0, 0.0), axis=0, keepdims=True).astype(I32)
        e = rrow.astype(I32)
        dz = (lax.shift_right_logical(e, 4) + SIDE - z) & 3
        dy = ((lax.shift_right_logical(e, 2) & 3) + SIDE - y) & 3
        dx = ((e & 3) + SIDE - x) & 3
        offset = dz * 16 + dy * 4 + dx
        place = jnp.zeros_like(offset)
        for (i, j, k), where in PLACE.items():
            place = jnp.where(offset == i * 16 + j * 4 + k, where, place)
        keys.append(place * SLOTS + rank)

    with jax.named_scope("meet"):
        pl.semaphore_wait(barrier, 3 * (SIDE - 1) + 2)
    with jax.named_scope("load_a"):
        for load in loads[1:3]:
            load.wait()
    halos = [
        remote(
            v.at[pl.ds(rows - 16, 16)], halo.at[i], halo_s.at[i], halo_r.at[i],
            sp=lax.rem(sp + 1, peers),
        )
        for i, v in enumerate((cin_v, gin_v))
    ]
    for copy in halos:
        copy.start()

    def tell(axis, i):
        for offset in lines[axis]:
            pl.semaphore_signal(
                known.at[i], inc=1, device_id={"sp": peer(offset)}, device_id_type=MESH
            )

    tell(1, 0)

    with jax.named_scope("load_b"):
        for load in loads[3:5]:
            load.wait()
    taps = taps_ref[...].astype(F32)
    t0, t1, t2 = taps[0:1], taps[1:2], taps[2:3]
    mixed = gin_v[...].astype(F32) * cin_v[...].astype(F32)
    row = iota(mixed.shape, 0)
    m1 = jnp.where(row < 1, 0.0, pltpu.roll(mixed, 1, 0))
    m2 = jnp.where(row < 2, 0.0, pltpu.roll(mixed, 2, 0))
    gated = (gout_v[...].astype(F32) * (t0 * m2 + t1 * m1 + t2 * mixed)).astype(BF16)
    with jax.named_scope("load_c"):
        loads[5].wait()
    with jax.named_scope("project"):
        part[...] = dot(gated, op_v[...])
    their_rows = pl.multiple_of(other * tok, tok)
    spans = [(0, 16), (16, tok - 16)]
    swaps = [
        remote(
            part.at[pl.ds(pl.multiple_of(their_rows + lo, 16), n)], pxr.at[pl.ds(lo, n)],
            px_s.at[i], px_r.at[i], tp=other,
        )
        for i, (lo, n) in enumerate(spans)
    ]
    swaps[1].start()

    @pl.when(tp == 0)
    def _():
        swaps[0].start()

    matrices = [(wg_h, wg_v), (wu_h, wu_v), (wd_h, wd_v)]
    for i, (src, dst) in enumerate(matrices):
        size = dst.shape[0] // 4
        for k in range(4):
            cut = pl.ds(k * size, size)
            pltpu.make_async_copy(src.at[0, cut], dst.at[cut], w_sem.at[i]).start()

    with jax.named_scope("known_0"):
        pl.semaphore_wait(known.at[0], SIDE - 1)
    tell(0, 1)

    a, b = iota((ROWS, ROWS), 0), iota((ROWS, ROWS), 1)
    slab_of = lax.shift_right_logical(a, 4) * SLOTS + (a & 3)
    quarter_ok = (lax.shift_right_logical(a, 2) & 3) == lax.shift_right_logical(b, 6)
    for g in range(GROUPS):
        want = slab_of + g * SLABS * SLOTS
        hit = ((keys[0] == want) | (keys[1] == want)) & quarter_ok
        picks[g] = jnp.where(hit, 1.0, 0.0).astype(BF16)

    def plain_to_slab(r):
        q, i, s = lax.shift_right_logical(r, 6), lax.shift_right_logical(r, 2) & 15, r & 3
        return i * 16 + q * 4 + s

    u_v[...] = jnp.where(plain_to_slab(a) == b, 1.0, 0.0).astype(BF16)
    ut_v[...] = jnp.where(plain_to_slab(b) == a, 1.0, 0.0).astype(BF16)
    for load in loads[6:]:
        load.wait()

    def first_rows():
        with jax.named_scope("halo"):
            for copy in halos:
                copy.wait()
        hm = jnp.where(sp > 0, halo[0].astype(F32) * halo[1].astype(F32), 0.0)
        ext = jnp.concatenate([hm, gin_v[0:16].astype(F32) * cin_v[0:16].astype(F32)], axis=0)
        conv = t0 * pltpu.roll(ext, 2, 0)[16:32] + t1 * pltpu.roll(ext, 1, 0)[16:32] + t2 * ext[16:32]
        with jax.named_scope("first"):
            part[0:16] = dot((gout_v[0:16].astype(F32) * conv).astype(BF16), op_v[...])

    def norm():
        with jax.named_scope("swap"):
            for copy in swaps:
                copy.wait_recv()
        s = part[pl.ds(pl.multiple_of(tp * tok, tok), tok)] + pxr[...] + res_v[...].astype(F32)
        stream[...] = s
        inverse = lax.rsqrt(jnp.mean(s * s, axis=-1, keepdims=True) + EPS)
        normed = (s * inverse * gain_ref[...]).astype(BF16)
        for q in range(QUARTERS):
            n4[q * tok : (q + 1) * tok] = normed[:, q * piece : (q + 1) * piece]

    base = tp * GROUPS * SLABS

    def dispatch(g):
        with jax.named_scope(f"pack_{g}"):
            send[g * SLABS : (g + 1) * SLABS] = dot(picks[g], n4[...]).astype(BF16).reshape(SLABS, 16, piece)
        for offset in far_first(g):
            pos = PLACE[offset]
            if distance(offset):
                remote(
                    send.at[pos], taken.at[base + pos], dsp_s, dsp_r.at[g], sp=peer(offset)
                ).start()
            else:
                pltpu.make_async_copy(send.at[pos], taken.at[base + pos], dsp_r.at[g]).start()

    @pl.when(tp == 1)
    def _():
        norm()
        pl.semaphore_wait(known.at[1], SIDE - 1)
        dispatch(0)
        dispatch(1)
        first_rows()
        swaps[0].start()
        dispatch(2)
        dispatch(3)

    @pl.when(tp == 0)
    def _():
        first_rows()
        norm()
        pl.semaphore_wait(known.at[1], SIDE - 1)
        for g in (2, 3, 0, 1):
            dispatch(g)

    def part_of(ref, g, core=0):
        return ref.at[pl.ds(core * GROUPS * SLABS + g * SLABS, SLABS)]

    def arrived(ref, sem, g):
        return remote(part_of(ref, g), part_of(ref, g), sem, sem, tp=other)

    def forward(g):
        return remote(part_of(taken, g, tp), part_of(taken, g, tp), fwd_s.at[g], fwd_r.at[g], tp=other)

    def half(core, g, rows=pl.ds(0, ROWS)):
        return remote(
            mine.at[core * GROUPS + g, rows], theirs.at[g, rows], pp_s.at[g], pp_r.at[g], tp=other
        )

    lane = iota((tok, ROWS), 1)
    lane_slot = lax.shift_right_logical(lane, 4) * SLOTS + (lane & 3)
    lane_quarter = lax.shift_right_logical(lane, 2) & 3
    weights = [upright(weight_ref[k : k + 1]) for k in range(2)]
    key_cols = [upright(k[:, :tok].astype(F32)).astype(I32) for k in keys]
    for g in range(GROUPS):
        want = lane_slot + g * SLABS * SLOTS
        mix = sum(jnp.where(k == want, w, 0.0) for k, w in zip(key_cols, weights))
        high = mix.astype(BF16).astype(F32)
        for i, m in enumerate((high, mix - high)):
            for q in range(QUARTERS):
                at = (i * QUARTERS + q) * tok
                mixes[g, at : at + tok] = jnp.where(lane_quarter == q, m, 0.0).astype(BF16)

    def take(core, g):
        @pl.when(tp == core)
        def _():
            with jax.named_scope(f"take_{core}_{g}"):
                arrived(taken, dsp_r.at[g], g).wait_recv()
            forward(g).start()

    def unpack(core, g, at):
        @pl.when(tp != core)
        def _():
            with jax.named_scope(f"other_{core}_{g}"):
                forward(g).wait_recv()

        start = (core * GROUPS + g) * SLABS
        with jax.named_scope(f"unpack_{core}_{g}"):
            plain = dot(u_v[...], taken[start : start + SLABS].reshape(ROWS, piece)).astype(BF16)
            for q in range(QUARTERS):
                x_v[at : at + tok, q * piece : (q + 1) * piece] = plain[q * tok : (q + 1) * tok]

    def give_back(core, groups):
        @pl.when(tp == core)
        def _():
            for g in groups:
                with jax.named_scope(f"half_{core}_{g}"):
                    half(core, g).wait_recv()
                with jax.named_scope(f"repack_{core}_{g}"):
                    total = (mine[core * GROUPS + g].astype(F32) + theirs[g].astype(F32)).astype(BF16)
                    slabs = dot(ut_v[...], total).astype(BF16)
                    rsend[g * SLABS : (g + 1) * SLABS] = slabs.reshape(SLABS, 16, piece)
                for offset in far_first(g):
                    pos = PLACE[offset]
                    if distance(offset):
                        remote(
                            rsend.at[pos], rret.at[pos], ret_s, ret_r.at[g], sp=peer(offset, -1)
                        ).start()
                    else:
                        pltpu.make_async_copy(rsend.at[pos], rret.at[pos], ret_r.at[g]).start()

    steps = [(1, (0, 1)), (1, (2, 3)), (0, (2, 3)), (0, (0, 1))]
    for g in steps[0][1]:
        take(1, g)
    for step, (core, groups) in enumerate(steps):
        for i, g in enumerate(groups):
            unpack(core, g, i * tok)
        if step == 0:
            with jax.named_scope("weights"):
                for i, (src, dst) in enumerate(matrices[:2]):
                    pltpu.make_async_copy(src.at[0], dst, w_sem.at[i]).wait()
        tiles = hidden // 256
        for n in range(tiles):
            cols = slice(n * 256, (n + 1) * 256)
            gate, up = dot(x_v[...], wg_v[:, cols]), dot(x_v[...], wu_v[:, cols])
            h_v[:, cols] = (gate / (1.0 + jnp.exp(-gate)) * up).astype(BF16)
            if n == tiles // 2 and step:
                give_back(*steps[step - 1])
            if n == (tiles - 1 if step == 1 else tiles // 2) and 0 < step < len(steps) - 1:
                for g in steps[step + 1][1]:
                    take(steps[step + 1][0], g)
        if step == 0:
            pltpu.make_async_copy(wd_h.at[0], wd_v, w_sem.at[2]).wait()
        for q in range(QUARTERS):
            res = dot(h_v[...], wd_v[:, q * piece : (q + 1) * piece]).astype(BF16)
            rows = slice(q * tok, (q + 1) * tok)
            for i, g in enumerate(groups):
                mine[core * GROUPS + g, rows] = res[i * tok : (i + 1) * tok]

            @pl.when(tp != core)
            def _():
                for g in groups:
                    half(core, g, pl.ds(q * tok, tok)).start()

        if step == 0:
            for g in steps[1][1]:
                take(steps[1][0], g)
    give_back(*steps[-1])

    comb[...] = jnp.zeros_like(comb)
    for g in (2, 3, 1, 0):
        with jax.named_scope(f"back_{g}"):
            arrived(rret, ret_r.at[g], g).wait_recv()
        slabs = rret[g * SLABS : (g + 1) * SLABS].reshape(ROWS, piece)
        comb[...] += dot(mixes[g], slabs)
    for q in range(QUARTERS):
        cols = slice(q * piece, (q + 1) * piece)
        routed = comb[q * tok : (q + 1) * tok] + comb[(QUARTERS + q) * tok : (QUARTERS + q + 1) * tok]
        out_ref[:, cols] = (stream[:, cols] + routed).astype(BF16)

    for copy in swaps:
        copy.wait_send()
    rest = pl.ds(1, GROUPS * SLABS - 1)
    remote(send.at[rest], rret.at[rest], dsp_s, dsp_s, tp=other).wait_send()
    remote(rsend.at[rest], rret.at[rest], ret_s, ret_s, tp=other).wait_send()
    for g in range(GROUPS):
        forward(g).wait_send()
        half(0, g).wait_send()


def per_device(
    residual, conv_input, input_gate, output_gate, conv_taps, out_proj, norm_gain, routes,
    route_weight, gate_proj, up_proj, down_proj,
):
    rows, chan = conv_input.shape
    tok, width = residual.shape
    hidden = gate_proj.shape[2]
    piece = width // QUARTERS
    slabs = (GROUPS * SLABS, QUARTERS * SLOTS, piece)
    hbm = pl.BlockSpec(memory_space=pltpu.HBM)
    dma = pltpu.SemaphoreType.DMA
    v = pltpu.VMEM
    return pl.pallas_call(
        kernel,
        out_shape=jax.ShapeDtypeStruct((tok, width), BF16),
        in_specs=[hbm] * 12,
        out_specs=pl.BlockSpec(memory_space=pltpu.VMEM),
        scratch_shapes=[
            v(conv_taps.shape, BF16), v((1, width), F32), v((2, tok), I32), v((2, tok), F32),
            v((rows, chan), BF16), v((rows, chan), BF16), v((rows, chan), BF16),
            v((tok, width), BF16), v((chan, width), BF16),
            v((width, hidden), BF16), v((width, hidden), BF16), v((hidden, width), BF16),
            v((2, 16, chan), BF16), v((rows, width), F32), v((tok, width), F32), v((tok, width), F32),
            v((QUARTERS * tok, piece), BF16),
            v(slabs, BF16), v((2 * slabs[0], *slabs[1:]), BF16), v(slabs, BF16), v(slabs, BF16),
            v((2 * tok, width), BF16), v((2 * tok, hidden), BF16),
            v((2 * GROUPS, ROWS, piece), BF16), v((GROUPS, ROWS, piece), BF16),
            v((ROWS, ROWS), BF16), v((ROWS, ROWS), BF16), v((GROUPS, ROWS, ROWS), BF16),
            v((GROUPS, 2 * ROWS, ROWS), BF16), v((2 * ROWS, piece), F32),
            pltpu.SemaphoreType.REGULAR((2,)), dma((9,)), dma((3,)), dma((2,)), dma((2,)), dma((2,)), dma((2,)),
            dma, dma((GROUPS,)), dma((GROUPS,)), dma((GROUPS,)), dma((GROUPS,)), dma((GROUPS,)),
            dma, dma((GROUPS,)),
        ],
        compiler_params=pltpu.CompilerParams(
            collective_id=0, has_side_effects=True, vmem_limit_bytes=60 * 2**20
        ),
        name="layer",
    )(
        residual, conv_input, input_gate, output_gate, conv_taps, out_proj, norm_gain.reshape(1, -1),
        routes.T, route_weight.T, gate_proj, up_proj, down_proj,
    )


def solution(mesh):
    return jax.shard_map(
        per_device,
        mesh=mesh,
        in_specs=(
            P(("sp", "tp"), None),
            P("sp", "tp"),
            P("sp", "tp"),
            P("sp", "tp"),
            P(None, "tp"),
            P("tp", None),
            P(),
            P(("sp", "tp"), None),
            P(("sp", "tp"), None),
            P("sp", None, "tp"),
            P("sp", None, "tp"),
            P("sp", "tp", None),
        ),
        out_specs=P(("sp", "tp"), None),
        check_vma=False,
    )
```

```python
import functools

import jax
import jax.numpy as jnp
from jax import lax
from jax.experimental import pallas as pl
from jax.experimental.pallas import tpu as pltpu
from jax.sharding import PartitionSpec as P

MESH = pl.DeviceIdType.MESH
F32, BF16, I32 = jnp.float32, jnp.bfloat16, jnp.int32
SIDE = 4
GROUPS = 4
SLABS = 16
SLOTS = 4
QUARTERS = 4
ROWS = SLABS * QUARTERS * SLOTS
EPS = 1e-06


def distance(offset):
    return sum(min(k, SIDE - k) for k in offset)


def peer_groups():
    every = [(i, j, k) for i in range(SIDE) for j in range(SIDE) for k in range(SIDE)]
    one_way = [o for o in every if distance(o) == 2 and (2 in o or set(o) in ({0, 1}, {0, 3}))]
    first = [o for o in every if distance(o) < 2] + one_way
    second = [o for o in every if distance(o) == 2 and o not in one_way]
    second += [o for o in every if distance(o) == 3 and 2 not in o] + [(2, 1, 0), (2, 3, 0)]
    far = sorted((o for o in every if o not in first and o not in second), key=distance)
    return [first, second, far[0::2], far[1::2]]


PEERS = peer_groups()
PLACE = {o: g * SLABS + i for g, members in enumerate(PEERS) for i, o in enumerate(members)}


def far_first(g):
    return sorted(PEERS[g], key=lambda o: -distance(o))


def iota(shape, dim):
    return lax.broadcasted_iota(I32, shape, dim)


def dot(a, b):
    return jnp.dot(a, b, preferred_element_type=F32)


def kernel(
    res_h, cin_h, gin_h, gout_h, taps_h, oproj_h, gain_h, routes_h, weight_h,
    wg_h, wu_h, wd_h, out_ref,
    taps_ref, gain_ref, routes_ref, weight_ref, cin_v, gin_v, gout_v, res_v, op_v, wg_v, wu_v, wd_v, halo, part, pxr, stream, n4,
    send, taken, rsend, rret, x_v, h_v, mine, theirs, u_v, ut_v, picks, mixes, comb,
    known, in_sem, w_sem, halo_s, halo_r, px_s, px_r, dsp_s, dsp_r, fwd_s, fwd_r, pp_s, pp_r, ret_s, ret_r,
):
    sp, tp = lax.axis_index("sp"), lax.axis_index("tp")
    z, y, x = lax.div(sp, 16), lax.rem(lax.div(sp, 4), 4), lax.rem(sp, 4)
    other = 1 - tp
    rows, tok = cin_v.shape[0], res_v.shape[0]
    width, hidden = out_ref.shape[1], h_v.shape[1]
    piece = width // QUARTERS

    def remote(src, dst, s, r, **where):
        return pltpu.make_async_remote_copy(
            src_ref=src, dst_ref=dst, send_sem=s, recv_sem=r, device_id=where, device_id_type=MESH
        )

    def peer(offset, sign=1):
        dz, dy, dx = (sign * k % SIDE for k in offset)
        return lax.rem(z + dz, SIDE) * 16 + lax.rem(y + dy, SIDE) * 4 + lax.rem(x + dx, SIDE)

    barrier = pltpu.get_barrier_semaphore()
    peers = SIDE**3
    lines = [[tuple(k if a == axis else 0 for a in range(3)) for k in range(1, SIDE)] for axis in range(3)]
    for line in lines:
        for offset in line:
            pl.semaphore_signal(barrier, inc=1, device_id={"sp": peer(offset)}, device_id_type=MESH)
    pl.semaphore_signal(barrier, inc=1, device_id={"tp": other}, device_id_type=MESH)
    pl.semaphore_signal(
        barrier, inc=1, device_id={"sp": lax.rem(sp + peers - 1, peers)}, device_id_type=MESH
    )

    loads = [
        pltpu.make_async_copy(a, b, in_sem.at[i])
        for i, (a, b) in enumerate(
            [
                (routes_h, routes_ref), (cin_h, cin_v), (gin_h, gin_v), (gout_h, gout_v),
                (taps_h, taps_ref), (oproj_h, op_v), (res_h, res_v), (gain_h, gain_ref),
                (weight_h, weight_ref),
            ]
        )
    ]
    for load in loads:
        load.start()
    lanes = QUARTERS * tok
    trow, tcol = iota((tok, lanes), 0), lax.rem(iota((tok, lanes), 1), tok)
    same, before = trow == tcol, trow < tcol
    loads[0].wait()
    diagonal = iota((tok, tok), 0) == iota((tok, tok), 1)

    def upright(line):
        return jnp.sum(jnp.where(diagonal, line, 0.0), axis=1, keepdims=True)

    cols = [upright(routes_ref[k : k + 1].astype(F32)) for k in range(2)]
    keys = []
    for rc in cols:
        rrow = jnp.sum(jnp.where(same, rc, 0.0), axis=0, keepdims=True)
        hits = ((cols[0] == rrow) | (cols[1] == rrow)) & before
        rank = jnp.sum(jnp.where(hits, 1.0, 0.0), axis=0, keepdims=True).astype(I32)
        e = rrow.astype(I32)
        dz = (lax.shift_right_logical(e, 4) + SIDE - z) & 3
        dy = ((lax.shift_right_logical(e, 2) & 3) + SIDE - y) & 3
        dx = ((e & 3) + SIDE - x) & 3
        offset = dz * 16 + dy * 4 + dx
        place = jnp.zeros_like(offset)
        for (i, j, k), where in PLACE.items():
            place = jnp.where(offset == i * 16 + j * 4 + k, where, place)
        keys.append(place * SLOTS + rank)

    with jax.named_scope("meet"):
        pl.semaphore_wait(barrier, 3 * (SIDE - 1) + 2)
    with jax.named_scope("load_a"):
        for load in loads[1:3]:
            load.wait()
    halos = [
        remote(
            v.at[pl.ds(rows - 16, 16)], halo.at[i], halo_s.at[i], halo_r.at[i],
            sp=lax.rem(sp + 1, peers),
        )
        for i, v in enumerate((cin_v, gin_v))
    ]
    for copy in halos:
        copy.start()

    def tell(axis, i):
        for offset in lines[axis]:
            pl.semaphore_signal(
                known.at[i], inc=1, device_id={"sp": peer(offset)}, device_id_type=MESH
            )

    tell(1, 0)

    with jax.named_scope("load_b"):
        for load in loads[3:5]:
            load.wait()
    taps = taps_ref[...].astype(F32)
    t0, t1, t2 = taps[0:1], taps[1:2], taps[2:3]
    mixed = gin_v[...].astype(F32) * cin_v[...].astype(F32)
    row = iota(mixed.shape, 0)
    m1 = jnp.where(row < 1, 0.0, pltpu.roll(mixed, 1, 0))
    m2 = jnp.where(row < 2, 0.0, pltpu.roll(mixed, 2, 0))
    gated = (gout_v[...].astype(F32) * (t0 * m2 + t1 * m1 + t2 * mixed)).astype(BF16)
    with jax.named_scope("load_c"):
        loads[5].wait()
    with jax.named_scope("project"):
        part[...] = dot(gated, op_v[...])
    their_rows = pl.multiple_of(other * tok, tok)
    spans = [(0, 16), (16, tok - 16)]
    swaps = [
        remote(
            part.at[pl.ds(pl.multiple_of(their_rows + lo, 16), n)], pxr.at[pl.ds(lo, n)],
            px_s.at[i], px_r.at[i], tp=other,
        )
        for i, (lo, n) in enumerate(spans)
    ]
    swaps[1].start()

    @pl.when(tp == 0)
    def _():
        swaps[0].start()

    matrices = [(wg_h, wg_v), (wu_h, wu_v), (wd_h, wd_v)]
    for i, (src, dst) in enumerate(matrices):
        size = dst.shape[0] // 4
        for k in range(4):
            cut = pl.ds(k * size, size)
            pltpu.make_async_copy(src.at[0, cut], dst.at[cut], w_sem.at[i]).start()

    with jax.named_scope("known_0"):
        pl.semaphore_wait(known.at[0], SIDE - 1)
    tell(0, 1)

    a, b = iota((ROWS, ROWS), 0), iota((ROWS, ROWS), 1)
    slab_of = lax.shift_right_logical(a, 4) * SLOTS + (a & 3)
    quarter_ok = (lax.shift_right_logical(a, 2) & 3) == lax.shift_right_logical(b, 6)
    for g in range(GROUPS):
        want = slab_of + g * SLABS * SLOTS
        hit = ((keys[0] == want) | (keys[1] == want)) & quarter_ok
        picks[g] = jnp.where(hit, 1.0, 0.0).astype(BF16)

    def plain_to_slab(r):
        q, i, s = lax.shift_right_logical(r, 6), lax.shift_right_logical(r, 2) & 15, r & 3
        return i * 16 + q * 4 + s

    u_v[...] = jnp.where(plain_to_slab(a) == b, 1.0, 0.0).astype(BF16)
    ut_v[...] = jnp.where(plain_to_slab(b) == a, 1.0, 0.0).astype(BF16)
    for load in loads[6:]:
        load.wait()

    def first_rows():
        with jax.named_scope("halo"):
            for copy in halos:
                copy.wait()
        hm = jnp.where(sp > 0, halo[0].astype(F32) * halo[1].astype(F32), 0.0)
        ext = jnp.concatenate([hm, gin_v[0:16].astype(F32) * cin_v[0:16].astype(F32)], axis=0)
        conv = t0 * pltpu.roll(ext, 2, 0)[16:32] + t1 * pltpu.roll(ext, 1, 0)[16:32] + t2 * ext[16:32]
        with jax.named_scope("first"):
            part[0:16] = dot((gout_v[0:16].astype(F32) * conv).astype(BF16), op_v[...])

    def norm():
        with jax.named_scope("swap"):
            for copy in swaps:
                copy.wait_recv()
        s = part[pl.ds(pl.multiple_of(tp * tok, tok), tok)] + pxr[...] + res_v[...].astype(F32)
        stream[...] = s
        inverse = lax.rsqrt(jnp.mean(s * s, axis=-1, keepdims=True) + EPS)
        normed = (s * inverse * gain_ref[...]).astype(BF16)
        for q in range(QUARTERS):
            n4[q * tok : (q + 1) * tok] = normed[:, q * piece : (q + 1) * piece]

    base = tp * GROUPS * SLABS

    def dispatch(g):
        with jax.named_scope(f"pack_{g}"):
            send[g * SLABS : (g + 1) * SLABS] = dot(picks[g], n4[...]).astype(BF16).reshape(SLABS, 16, piece)
        for offset in far_first(g):
            pos = PLACE[offset]
            if distance(offset):
                remote(
                    send.at[pos], taken.at[base + pos], dsp_s, dsp_r.at[g], sp=peer(offset)
                ).start()
            else:
                pltpu.make_async_copy(send.at[pos], taken.at[base + pos], dsp_r.at[g]).start()

    @pl.when(tp == 1)
    def _():
        norm()
        pl.semaphore_wait(known.at[1], SIDE - 1)
        dispatch(0)
        dispatch(1)
        first_rows()
        swaps[0].start()
        dispatch(2)
        dispatch(3)

    @pl.when(tp == 0)
    def _():
        first_rows()
        norm()
        pl.semaphore_wait(known.at[1], SIDE - 1)
        pl.semaphore_wait(known.at[2], 1)
        for g in (2, 3, 0, 1):
            dispatch(g)

    def part_of(ref, g, core=0):
        return ref.at[pl.ds(core * GROUPS * SLABS + g * SLABS, SLABS)]

    def arrived(ref, sem, g):
        return remote(part_of(ref, g), part_of(ref, g), sem, sem, tp=other)

    def forward(g):
        return remote(part_of(taken, g, tp), part_of(taken, g, tp), fwd_s.at[g], fwd_r.at[g], tp=other)

    def half(core, g, rows=pl.ds(0, ROWS)):
        return remote(
            mine.at[core * GROUPS + g, rows], theirs.at[g, rows], pp_s.at[g], pp_r.at[g], tp=other
        )

    lane = iota((tok, ROWS), 1)
    lane_slot = lax.shift_right_logical(lane, 4) * SLOTS + (lane & 3)
    lane_quarter = lax.shift_right_logical(lane, 2) & 3
    weights = [upright(weight_ref[k : k + 1]) for k in range(2)]
    key_cols = [upright(k[:, :tok].astype(F32)).astype(I32) for k in keys]
    for g in range(GROUPS):
        want = lane_slot + g * SLABS * SLOTS
        mix = sum(jnp.where(k == want, w, 0.0) for k, w in zip(key_cols, weights))
        high = mix.astype(BF16).astype(F32)
        for i, m in enumerate((high, mix - high)):
            for q in range(QUARTERS):
                at = (i * QUARTERS + q) * tok
                mixes[g, at : at + tok] = jnp.where(lane_quarter == q, m, 0.0).astype(BF16)

    def take(core, g):
        @pl.when(tp == core)
        def _():
            with jax.named_scope(f"take_{core}_{g}"):
                arrived(taken, dsp_r.at[g], g).wait_recv()
            forward(g).start()

    def unpack(core, g, at):
        @pl.when(tp != core)
        def _():
            with jax.named_scope(f"other_{core}_{g}"):
                forward(g).wait_recv()

        start = (core * GROUPS + g) * SLABS
        with jax.named_scope(f"unpack_{core}_{g}"):
            plain = dot(u_v[...], taken[start : start + SLABS].reshape(ROWS, piece)).astype(BF16)
            for q in range(QUARTERS):
                x_v[at : at + tok, q * piece : (q + 1) * piece] = plain[q * tok : (q + 1) * tok]

    def give_back(core, groups):
        @pl.when(tp == core)
        def _():
            for g in groups:
                with jax.named_scope(f"half_{core}_{g}"):
                    half(core, g).wait_recv()
                with jax.named_scope(f"repack_{core}_{g}"):
                    total = (mine[core * GROUPS + g].astype(F32) + theirs[g].astype(F32)).astype(BF16)
                    slabs = dot(ut_v[...], total).astype(BF16)
                    rsend[g * SLABS : (g + 1) * SLABS] = slabs.reshape(SLABS, 16, piece)
                for offset in far_first(g):
                    pos = PLACE[offset]
                    if distance(offset):
                        remote(
                            rsend.at[pos], rret.at[pos], ret_s, ret_r.at[g], sp=peer(offset, -1)
                        ).start()
                    else:
                        pltpu.make_async_copy(rsend.at[pos], rret.at[pos], ret_r.at[g]).start()

    steps = [(1, (0, 1)), (1, (2, 3)), (0, (2, 3)), (0, (0, 1))]
    take(1, 0)

    @pl.when(tp == 1)
    def _():
        pl.semaphore_signal(known.at[2], inc=1, device_id={"tp": other}, device_id_type=MESH)

    take(1, 1)
    for step, (core, groups) in enumerate(steps):
        for i, g in enumerate(groups):
            unpack(core, g, i * tok)
        if step == 0:
            with jax.named_scope("weights"):
                for i, (src, dst) in enumerate(matrices[:2]):
                    pltpu.make_async_copy(src.at[0], dst, w_sem.at[i]).wait()
        tiles = hidden // 256
        for n in range(tiles):
            cols = slice(n * 256, (n + 1) * 256)
            gate, up = dot(x_v[...], wg_v[:, cols]), dot(x_v[...], wu_v[:, cols])
            h_v[:, cols] = (gate / (1.0 + jnp.exp(-gate)) * up).astype(BF16)
            if n == tiles // 2 and step:
                give_back(*steps[step - 1])
            if n == (tiles - 1 if step == 1 else tiles // 2) and 0 < step < len(steps) - 1:
                for g in steps[step + 1][1]:
                    take(steps[step + 1][0], g)
        if step == 0:
            pltpu.make_async_copy(wd_h.at[0], wd_v, w_sem.at[2]).wait()
        for q in range(QUARTERS):
            res = dot(h_v[...], wd_v[:, q * piece : (q + 1) * piece]).astype(BF16)
            rows = slice(q * tok, (q + 1) * tok)
            for i, g in enumerate(groups):
                mine[core * GROUPS + g, rows] = res[i * tok : (i + 1) * tok]

            if q == QUARTERS - 1 or (q == QUARTERS // 2 - 1 and step == len(steps) - 1):
                since = 0 if q < QUARTERS - 1 or step < len(steps) - 1 else QUARTERS // 2

                @pl.when(tp != core)
                def _():
                    for g in groups:
                        half(core, g, pl.ds(since * tok, (q + 1 - since) * tok)).start()

        if step == 0:
            for g in steps[1][1]:
                take(steps[1][0], g)
    give_back(*steps[-1])

    comb[...] = jnp.zeros_like(comb)
    for g in (2, 3, 1, 0):
        with jax.named_scope(f"back_{g}"):
            arrived(rret, ret_r.at[g], g).wait_recv()
        slabs = rret[g * SLABS : (g + 1) * SLABS].reshape(ROWS, piece)
        comb[...] += dot(mixes[g], slabs)
    for q in range(QUARTERS):
        cols = slice(q * piece, (q + 1) * piece)
        routed = comb[q * tok : (q + 1) * tok] + comb[(QUARTERS + q) * tok : (QUARTERS + q + 1) * tok]
        out_ref[:, cols] = (stream[:, cols] + routed).astype(BF16)

    for copy in swaps:
        copy.wait_send()
    rest = pl.ds(1, GROUPS * SLABS - 1)
    remote(send.at[rest], rret.at[rest], dsp_s, dsp_s, tp=other).wait_send()
    remote(rsend.at[rest], rret.at[rest], ret_s, ret_s, tp=other).wait_send()
    for g in range(GROUPS):
        forward(g).wait_send()
        half(0, g).wait_send()


def per_device(
    residual, conv_input, input_gate, output_gate, conv_taps, out_proj, norm_gain, routes,
    route_weight, gate_proj, up_proj, down_proj,
):
    rows, chan = conv_input.shape
    tok, width = residual.shape
    hidden = gate_proj.shape[2]
    piece = width // QUARTERS
    slabs = (GROUPS * SLABS, QUARTERS * SLOTS, piece)
    hbm = pl.BlockSpec(memory_space=pltpu.HBM)
    dma = pltpu.SemaphoreType.DMA
    v = pltpu.VMEM
    return pl.pallas_call(
        kernel,
        out_shape=jax.ShapeDtypeStruct((tok, width), BF16),
        in_specs=[hbm] * 12,
        out_specs=pl.BlockSpec(memory_space=pltpu.VMEM),
        scratch_shapes=[
            v(conv_taps.shape, BF16), v((1, width), F32), v((2, tok), I32), v((2, tok), F32),
            v((rows, chan), BF16), v((rows, chan), BF16), v((rows, chan), BF16),
            v((tok, width), BF16), v((chan, width), BF16),
            v((width, hidden), BF16), v((width, hidden), BF16), v((hidden, width), BF16),
            v((2, 16, chan), BF16), v((rows, width), F32), v((tok, width), F32), v((tok, width), F32),
            v((QUARTERS * tok, piece), BF16),
            v(slabs, BF16), v((2 * slabs[0], *slabs[1:]), BF16), v(slabs, BF16), v(slabs, BF16),
            v((2 * tok, width), BF16), v((2 * tok, hidden), BF16),
            v((2 * GROUPS, ROWS, piece), BF16), v((GROUPS, ROWS, piece), BF16),
            v((ROWS, ROWS), BF16), v((ROWS, ROWS), BF16), v((GROUPS, ROWS, ROWS), BF16),
            v((GROUPS, 2 * ROWS, ROWS), BF16), v((2 * ROWS, piece), F32),
            pltpu.SemaphoreType.REGULAR((3,)), dma((9,)), dma((3,)), dma((2,)), dma((2,)), dma((2,)), dma((2,)),
            dma, dma((GROUPS,)), dma((GROUPS,)), dma((GROUPS,)), dma((GROUPS,)), dma((GROUPS,)),
            dma, dma((GROUPS,)),
        ],
        compiler_params=pltpu.CompilerParams(
            collective_id=0, has_side_effects=True, vmem_limit_bytes=60 * 2**20
        ),
        name="layer",
    )(
        residual, conv_input, input_gate, output_gate, conv_taps, out_proj, norm_gain.reshape(1, -1),
        routes.T, route_weight.T, gate_proj, up_proj, down_proj,
    )


def solution(mesh):
    return jax.shard_map(
        per_device,
        mesh=mesh,
        in_specs=(
            P(("sp", "tp"), None),
            P("sp", "tp"),
            P("sp", "tp"),
            P("sp", "tp"),
            P(None, "tp"),
            P("tp", None),
            P(),
            P(("sp", "tp"), None),
            P(("sp", "tp"), None),
            P("sp", None, "tp"),
            P("sp", None, "tp"),
            P("sp", "tp", None),
        ),
        out_specs=P(("sp", "tp"), None),
        check_vma=False,
    )
```

```python
import functools

import jax
import jax.numpy as jnp
from jax import lax
from jax.experimental import pallas as pl
from jax.experimental.pallas import tpu as pltpu
from jax.sharding import PartitionSpec as P

MESH = pl.DeviceIdType.MESH
F32, BF16, I32 = jnp.float32, jnp.bfloat16, jnp.int32
SIDE = 4
GROUPS = 4
SLABS = 16
SLOTS = 4
QUARTERS = 4
ROWS = SLABS * QUARTERS * SLOTS
EPS = 1e-06


def distance(offset):
    return sum(min(k, SIDE - k) for k in offset)


def peer_groups():
    every = [(i, j, k) for i in range(SIDE) for j in range(SIDE) for k in range(SIDE)]
    one_way = [o for o in every if distance(o) == 2 and (2 in o or set(o) in ({0, 1}, {0, 3}))]
    first = [o for o in every if distance(o) < 2] + one_way
    second = [o for o in every if distance(o) == 2 and o not in one_way]
    second += [o for o in every if distance(o) == 3 and 2 not in o] + [(2, 1, 0), (2, 3, 0)]
    far = sorted((o for o in every if o not in first and o not in second), key=distance)
    return [first, second, far[0::2], far[1::2]]


PEERS = peer_groups()
PLACE = {o: g * SLABS + i for g, members in enumerate(PEERS) for i, o in enumerate(members)}


def far_first(g):
    return sorted(PEERS[g], key=lambda o: -distance(o))


def iota(shape, dim):
    return lax.broadcasted_iota(I32, shape, dim)


def dot(a, b):
    return jnp.dot(a, b, preferred_element_type=F32)


def kernel(
    res_h, cin_h, gin_h, gout_h, taps_h, oproj_h, gain_h, routes_h, weight_h,
    wg_h, wu_h, wd_h, out_ref,
    taps_ref, gain_ref, routes_ref, weight_ref, cin_v, gin_v, gout_v, res_v, op_v, wg_v, wu_v, wd_v, halo, part, pxr, stream, n4,
    send, taken, rsend, rret, x_v, h_v, mine, theirs, u_v, ut_v, picks, mixes, comb,
    known, in_sem, w_sem, halo_s, halo_r, px_s, px_r, dsp_s, dsp_r, fwd_s, fwd_r, pp_s, pp_r, ret_s, ret_r,
):
    sp, tp = lax.axis_index("sp"), lax.axis_index("tp")
    z, y, x = lax.div(sp, 16), lax.rem(lax.div(sp, 4), 4), lax.rem(sp, 4)
    other = 1 - tp
    rows, tok = cin_v.shape[0], res_v.shape[0]
    width, hidden = out_ref.shape[1], h_v.shape[1]
    piece = width // QUARTERS

    def remote(src, dst, s, r, **where):
        return pltpu.make_async_remote_copy(
            src_ref=src, dst_ref=dst, send_sem=s, recv_sem=r, device_id=where, device_id_type=MESH
        )

    def peer(offset, sign=1):
        dz, dy, dx = (sign * k % SIDE for k in offset)
        return lax.rem(z + dz, SIDE) * 16 + lax.rem(y + dy, SIDE) * 4 + lax.rem(x + dx, SIDE)

    barrier = pltpu.get_barrier_semaphore()
    peers = SIDE**3
    lines = [[tuple(k if a == axis else 0 for a in range(3)) for k in range(1, SIDE)] for axis in range(3)]
    for line in lines:
        for offset in line:
            pl.semaphore_signal(barrier, inc=1, device_id={"sp": peer(offset)}, device_id_type=MESH)
    pl.semaphore_signal(barrier, inc=1, device_id={"tp": other}, device_id_type=MESH)
    pl.semaphore_signal(
        barrier, inc=1, device_id={"sp": lax.rem(sp + peers - 1, peers)}, device_id_type=MESH
    )

    loads = [
        pltpu.make_async_copy(a, b, in_sem.at[i])
        for i, (a, b) in enumerate(
            [
                (routes_h, routes_ref), (cin_h, cin_v), (gin_h, gin_v), (gout_h, gout_v),
                (taps_h, taps_ref), (oproj_h, op_v), (res_h, res_v), (gain_h, gain_ref),
                (weight_h, weight_ref),
            ]
        )
    ]
    for load in loads:
        load.start()
    lanes = QUARTERS * tok
    trow, tcol = iota((tok, lanes), 0), lax.rem(iota((tok, lanes), 1), tok)
    same, before = trow == tcol, trow < tcol
    loads[0].wait()
    diagonal = iota((tok, tok), 0) == iota((tok, tok), 1)

    def upright(line):
        return jnp.sum(jnp.where(diagonal, line, 0.0), axis=1, keepdims=True)

    cols = [upright(routes_ref[k : k + 1].astype(F32)) for k in range(2)]
    keys = []
    for rc in cols:
        rrow = jnp.sum(jnp.where(same, rc, 0.0), axis=0, keepdims=True)
        hits = ((cols[0] == rrow) | (cols[1] == rrow)) & before
        rank = jnp.sum(jnp.where(hits, 1.0, 0.0), axis=0, keepdims=True).astype(I32)
        e = rrow.astype(I32)
        dz = (lax.shift_right_logical(e, 4) + SIDE - z) & 3
        dy = ((lax.shift_right_logical(e, 2) & 3) + SIDE - y) & 3
        dx = ((e & 3) + SIDE - x) & 3
        offset = dz * 16 + dy * 4 + dx
        place = jnp.zeros_like(offset)
        for (i, j, k), where in PLACE.items():
            place = jnp.where(offset == i * 16 + j * 4 + k, where, place)
        keys.append(place * SLOTS + rank)

    with jax.named_scope("meet"):
        pl.semaphore_wait(barrier, 3 * (SIDE - 1) + 2)
    with jax.named_scope("load_a"):
        for load in loads[1:3]:
            load.wait()
    halos = [
        remote(
            v.at[pl.ds(rows - 16, 16)], halo.at[i], halo_s.at[i], halo_r.at[i],
            sp=lax.rem(sp + 1, peers),
        )
        for i, v in enumerate((cin_v, gin_v))
    ]
    for copy in halos:
        copy.start()

    def tell(axis, i):
        for offset in lines[axis]:
            pl.semaphore_signal(
                known.at[i], inc=1, device_id={"sp": peer(offset)}, device_id_type=MESH
            )

    tell(1, 0)

    with jax.named_scope("load_b"):
        for load in loads[3:5]:
            load.wait()
    taps = taps_ref[...].astype(F32)
    t0, t1, t2 = taps[0:1], taps[1:2], taps[2:3]
    mixed = gin_v[...].astype(F32) * cin_v[...].astype(F32)
    row = iota(mixed.shape, 0)
    m1 = jnp.where(row < 1, 0.0, pltpu.roll(mixed, 1, 0))
    m2 = jnp.where(row < 2, 0.0, pltpu.roll(mixed, 2, 0))
    gated = (gout_v[...].astype(F32) * (t0 * m2 + t1 * m1 + t2 * mixed)).astype(BF16)
    with jax.named_scope("load_c"):
        loads[5].wait()
    with jax.named_scope("project"):
        part[...] = dot(gated, op_v[...])
    their_rows = pl.multiple_of(other * tok, tok)
    spans = [(0, 16), (16, tok - 16)]
    swaps = [
        remote(
            part.at[pl.ds(pl.multiple_of(their_rows + lo, 16), n)], pxr.at[pl.ds(lo, n)],
            px_s.at[i], px_r.at[i], tp=other,
        )
        for i, (lo, n) in enumerate(spans)
    ]
    swaps[1].start()

    @pl.when(tp == 0)
    def _():
        swaps[0].start()

    matrices = [(wg_h, wg_v), (wu_h, wu_v), (wd_h, wd_v)]
    for i, (src, dst) in enumerate(matrices):
        size = dst.shape[0] // 4
        for k in range(4):
            cut = pl.ds(k * size, size)
            pltpu.make_async_copy(src.at[0, cut], dst.at[cut], w_sem.at[i]).start()

    with jax.named_scope("known_0"):
        pl.semaphore_wait(known.at[0], SIDE - 1)
    tell(0, 1)

    a, b = iota((ROWS, ROWS), 0), iota((ROWS, ROWS), 1)
    slab_of = lax.shift_right_logical(a, 4) * SLOTS + (a & 3)
    quarter_ok = (lax.shift_right_logical(a, 2) & 3) == lax.shift_right_logical(b, 6)
    for g in range(GROUPS):
        want = slab_of + g * SLABS * SLOTS
        hit = ((keys[0] == want) | (keys[1] == want)) & quarter_ok
        picks[g] = jnp.where(hit, 1.0, 0.0).astype(BF16)

    def plain_to_slab(r):
        q, i, s = lax.shift_right_logical(r, 6), lax.shift_right_logical(r, 2) & 15, r & 3
        return i * 16 + q * 4 + s

    u_v[...] = jnp.where(plain_to_slab(a) == b, 1.0, 0.0).astype(BF16)
    ut_v[...] = jnp.where(plain_to_slab(b) == a, 1.0, 0.0).astype(BF16)
    for load in loads[6:]:
        load.wait()

    def first_rows():
        with jax.named_scope("halo"):
            for copy in halos:
                copy.wait()
        hm = jnp.where(sp > 0, halo[0].astype(F32) * halo[1].astype(F32), 0.0)
        ext = jnp.concatenate([hm, gin_v[0:16].astype(F32) * cin_v[0:16].astype(F32)], axis=0)
        conv = t0 * pltpu.roll(ext, 2, 0)[16:32] + t1 * pltpu.roll(ext, 1, 0)[16:32] + t2 * ext[16:32]
        with jax.named_scope("first"):
            part[0:16] = dot((gout_v[0:16].astype(F32) * conv).astype(BF16), op_v[...])

    def norm():
        with jax.named_scope("swap"):
            for copy in swaps:
                copy.wait_recv()
        s = part[pl.ds(pl.multiple_of(tp * tok, tok), tok)] + pxr[...] + res_v[...].astype(F32)
        stream[...] = s
        inverse = lax.rsqrt(jnp.mean(s * s, axis=-1, keepdims=True) + EPS)
        normed = (s * inverse * gain_ref[...]).astype(BF16)
        for q in range(QUARTERS):
            n4[q * tok : (q + 1) * tok] = normed[:, q * piece : (q + 1) * piece]

    base = tp * GROUPS * SLABS

    def dispatch(g):
        with jax.named_scope(f"pack_{g}"):
            send[g * SLABS : (g + 1) * SLABS] = dot(picks[g], n4[...]).astype(BF16).reshape(SLABS, 16, piece)
        for offset in far_first(g):
            pos = PLACE[offset]
            if distance(offset):
                remote(
                    send.at[pos], taken.at[base + pos], dsp_s, dsp_r.at[g], sp=peer(offset)
                ).start()
            else:
                pltpu.make_async_copy(send.at[pos], taken.at[base + pos], dsp_r.at[g]).start()

    @pl.when(tp == 1)
    def _():
        norm()
        pl.semaphore_wait(known.at[1], SIDE - 1)
        dispatch(0)
        dispatch(1)
        first_rows()
        swaps[0].start()
        dispatch(2)
        dispatch(3)

    @pl.when(tp == 0)
    def _():
        first_rows()
        norm()
        pl.semaphore_wait(known.at[1], SIDE - 1)
        pl.semaphore_wait(known.at[2], 1)
        for g in (2, 3, 0, 1):
            dispatch(g)

    def part_of(ref, g, core=0):
        return ref.at[pl.ds(core * GROUPS * SLABS + g * SLABS, SLABS)]

    def arrived(ref, sem, g):
        return remote(part_of(ref, g), part_of(ref, g), sem, sem, tp=other)

    def forward(g):
        return remote(part_of(taken, g, tp), part_of(taken, g, tp), fwd_s.at[g], fwd_r.at[g], tp=other)

    def half(core, g, rows=pl.ds(0, ROWS)):
        return remote(
            mine.at[core * GROUPS + g, rows], theirs.at[g, rows], pp_s.at[g], pp_r.at[g], tp=other
        )

    lane = iota((tok, ROWS), 1)
    lane_slot = lax.shift_right_logical(lane, 4) * SLOTS + (lane & 3)
    lane_quarter = lax.shift_right_logical(lane, 2) & 3
    weights = [upright(weight_ref[k : k + 1]) for k in range(2)]
    key_cols = [upright(k[:, :tok].astype(F32)).astype(I32) for k in keys]
    for g in range(GROUPS):
        want = lane_slot + g * SLABS * SLOTS
        mix = sum(jnp.where(k == want, w, 0.0) for k, w in zip(key_cols, weights))
        high = mix.astype(BF16).astype(F32)
        for i, m in enumerate((high, mix - high)):
            for q in range(QUARTERS):
                at = (i * QUARTERS + q) * tok
                mixes[g, at : at + tok] = jnp.where(lane_quarter == q, m, 0.0).astype(BF16)

    def take(core, g):
        @pl.when(tp == core)
        def _():
            with jax.named_scope(f"take_{core}_{g}"):
                arrived(taken, dsp_r.at[g], g).wait_recv()
            forward(g).start()

    def unpack(core, g, at):
        @pl.when(tp != core)
        def _():
            with jax.named_scope(f"other_{core}_{g}"):
                forward(g).wait_recv()

        start = (core * GROUPS + g) * SLABS
        with jax.named_scope(f"unpack_{core}_{g}"):
            plain = dot(u_v[...], taken[start : start + SLABS].reshape(ROWS, piece)).astype(BF16)
            for q in range(QUARTERS):
                x_v[at : at + tok, q * piece : (q + 1) * piece] = plain[q * tok : (q + 1) * tok]

    def give_back(core, groups):
        @pl.when(tp == core)
        def _():
            for g in groups:
                with jax.named_scope(f"half_{core}_{g}"):
                    half(core, g).wait_recv()
                with jax.named_scope(f"repack_{core}_{g}"):
                    total = (mine[core * GROUPS + g].astype(F32) + theirs[g].astype(F32)).astype(BF16)
                    slabs = dot(ut_v[...], total).astype(BF16)
                    rsend[g * SLABS : (g + 1) * SLABS] = slabs.reshape(SLABS, 16, piece)
                for offset in far_first(g):
                    pos = PLACE[offset]
                    if distance(offset):
                        remote(
                            rsend.at[pos], rret.at[pos], ret_s, ret_r.at[g], sp=peer(offset, -1)
                        ).start()
                    else:
                        pltpu.make_async_copy(rsend.at[pos], rret.at[pos], ret_r.at[g]).start()

    steps = [(1, (0, 1)), (1, (2, 3)), (0, (2, 3)), (0, (0, 1))]
    take(1, 0)

    @pl.when(tp == 1)
    def _():
        pl.semaphore_signal(known.at[2], inc=1, device_id={"tp": other}, device_id_type=MESH)

    take(1, 1)
    for step, (core, groups) in enumerate(steps):
        for i, g in enumerate(groups):
            unpack(core, g, i * tok)
        if step == 0:
            with jax.named_scope("weights"):
                for i, (src, dst) in enumerate(matrices[:2]):
                    pltpu.make_async_copy(src.at[0], dst, w_sem.at[i]).wait()
        tiles = hidden // 256
        for n in range(tiles):
            cols = slice(n * 256, (n + 1) * 256)
            gate, up = dot(x_v[...], wg_v[:, cols]), dot(x_v[...], wu_v[:, cols])
            h_v[:, cols] = (gate / (1.0 + jnp.exp(-gate)) * up).astype(BF16)
            if n == (2 if step == 3 else tiles // 2) and step:
                give_back(*steps[step - 1])
            if n == (tiles - 1 if step == 1 else tiles // 2) and 0 < step < len(steps) - 1:
                for g in steps[step + 1][1]:
                    take(steps[step + 1][0], g)
        if step == 0:
            pltpu.make_async_copy(wd_h.at[0], wd_v, w_sem.at[2]).wait()
        for q in range(QUARTERS):
            res = dot(h_v[...], wd_v[:, q * piece : (q + 1) * piece]).astype(BF16)
            rows = slice(q * tok, (q + 1) * tok)
            for i, g in enumerate(groups):
                mine[core * GROUPS + g, rows] = res[i * tok : (i + 1) * tok]

            if q == QUARTERS - 1 or (q == QUARTERS // 2 - 1 and step >= 2):
                since = 0 if q < QUARTERS - 1 or step < 2 else QUARTERS // 2

                @pl.when(tp != core)
                def _():
                    for g in groups:
                        half(core, g, pl.ds(since * tok, (q + 1 - since) * tok)).start()

        if step == 0:
            for g in steps[1][1]:
                take(steps[1][0], g)
    give_back(*steps[-1])

    comb[...] = jnp.zeros_like(comb)
    for g in (2, 3, 1, 0):
        with jax.named_scope(f"back_{g}"):
            arrived(rret, ret_r.at[g], g).wait_recv()
        slabs = rret[g * SLABS : (g + 1) * SLABS].reshape(ROWS, piece)
        comb[...] += dot(mixes[g], slabs)
    for q in range(QUARTERS):
        cols = slice(q * piece, (q + 1) * piece)
        routed = comb[q * tok : (q + 1) * tok] + comb[(QUARTERS + q) * tok : (QUARTERS + q + 1) * tok]
        out_ref[:, cols] = (stream[:, cols] + routed).astype(BF16)

    for copy in swaps:
        copy.wait_send()
    rest = pl.ds(1, GROUPS * SLABS - 1)
    remote(send.at[rest], rret.at[rest], dsp_s, dsp_s, tp=other).wait_send()
    remote(rsend.at[rest], rret.at[rest], ret_s, ret_s, tp=other).wait_send()
    for g in range(GROUPS):
        forward(g).wait_send()
        half(0, g).wait_send()


def per_device(
    residual, conv_input, input_gate, output_gate, conv_taps, out_proj, norm_gain, routes,
    route_weight, gate_proj, up_proj, down_proj,
):
    rows, chan = conv_input.shape
    tok, width = residual.shape
    hidden = gate_proj.shape[2]
    piece = width // QUARTERS
    slabs = (GROUPS * SLABS, QUARTERS * SLOTS, piece)
    hbm = pl.BlockSpec(memory_space=pltpu.HBM)
    dma = pltpu.SemaphoreType.DMA
    v = pltpu.VMEM
    return pl.pallas_call(
        kernel,
        out_shape=jax.ShapeDtypeStruct((tok, width), BF16),
        in_specs=[hbm] * 12,
        out_specs=pl.BlockSpec(memory_space=pltpu.VMEM),
        scratch_shapes=[
            v(conv_taps.shape, BF16), v((1, width), F32), v((2, tok), I32), v((2, tok), F32),
            v((rows, chan), BF16), v((rows, chan), BF16), v((rows, chan), BF16),
            v((tok, width), BF16), v((chan, width), BF16),
            v((width, hidden), BF16), v((width, hidden), BF16), v((hidden, width), BF16),
            v((2, 16, chan), BF16), v((rows, width), F32), v((tok, width), F32), v((tok, width), F32),
            v((QUARTERS * tok, piece), BF16),
            v(slabs, BF16), v((2 * slabs[0], *slabs[1:]), BF16), v(slabs, BF16), v(slabs, BF16),
            v((2 * tok, width), BF16), v((2 * tok, hidden), BF16),
            v((2 * GROUPS, ROWS, piece), BF16), v((GROUPS, ROWS, piece), BF16),
            v((ROWS, ROWS), BF16), v((ROWS, ROWS), BF16), v((GROUPS, ROWS, ROWS), BF16),
            v((GROUPS, 2 * ROWS, ROWS), BF16), v((2 * ROWS, piece), F32),
            pltpu.SemaphoreType.REGULAR((3,)), dma((9,)), dma((3,)), dma((2,)), dma((2,)), dma((2,)), dma((2,)),
            dma, dma((GROUPS,)), dma((GROUPS,)), dma((GROUPS,)), dma((GROUPS,)), dma((GROUPS,)),
            dma, dma((GROUPS,)),
        ],
        compiler_params=pltpu.CompilerParams(
            collective_id=0, has_side_effects=True, vmem_limit_bytes=60 * 2**20
        ),
        name="layer",
    )(
        residual, conv_input, input_gate, output_gate, conv_taps, out_proj, norm_gain.reshape(1, -1),
        routes.T, route_weight.T, gate_proj, up_proj, down_proj,
    )


def solution(mesh):
    return jax.shard_map(
        per_device,
        mesh=mesh,
        in_specs=(
            P(("sp", "tp"), None),
            P("sp", "tp"),
            P("sp", "tp"),
            P("sp", "tp"),
            P(None, "tp"),
            P("tp", None),
            P(),
            P(("sp", "tp"), None),
            P(("sp", "tp"), None),
            P("sp", None, "tp"),
            P("sp", None, "tp"),
            P("sp", "tp", None),
        ),
        out_specs=P(("sp", "tp"), None),
        check_vma=False,
    )
```
